32 devices in a mesh: sp: 8 (over z, y), tp: 4 (over x, core).
Axes of the slice: x: 2, y: 2, z: 4, core: 2. Of those that a mesh axis runs over, the one named last changes fastest.
Arguments:
- tokens: bfloat16 [6144, 4096], P('sp', 'tp'), may hold values from -6 to 6
- in_proj: bfloat16 [3, 4096, 1024], P(None, 'tp', 'sp'), may hold values from -0.09375 to 0.09375
- group_mix: bfloat16 [3, 4, 256, 256], replicated, may hold values from -0.375 to 0.375
- pool_gain: float32 [3, 1024], replicated, may hold values from 0.1 to 1.9
- out_proj: bfloat16 [3, 1024, 4096], P(None, 'sp', 'tp'), may hold values from -0.1875 to 0.1875
- norm_gain: float32 [3, 4096], P(None, 'tp'), may hold values from 0.25 to 3
- norm_bias: float32 [3, 4096], P(None, 'tp'), may hold values from -1.5 to 1.5
Outputs:
- stream_out: bfloat16 [6144, 4096], P('sp', 'tp')
The draws below stay inside these ranges and needn't reach their ends.
All inputs are finite; a program needn't handle non-finite values.
Results may differ from the reference program's by a relative error of at most 0.017.
Values may be sent and summed in bfloat16 or wider, within the bound.
A program may use at most 128 MiB of HBM per device.

```python
import jax
import jax.numpy as jnp
from jax import lax

D = 4096
P_SIZE = 1024
POOL_CH = 256
LAYERS = 3
SEQ = 6144
N_TP = 4


def draw_norm_gain(key, part):
    key_block, key_noise = jax.random.split(jax.random.fold_in(key, 17))
    block_scale = jnp.exp(jax.random.uniform(key_block, (LAYERS, 8, 1), jnp.float32, -0.7, 0.7))
    noise = 0.18 * jnp.clip(jax.random.normal(key_noise, (LAYERS, 8, D // 8), jnp.float32), -2.5, 2.5)
    return (block_scale * (1.0 + noise)).reshape(LAYERS, D)


def levels(key, dims, cuts, low, top_value):
    def one(dim, parts):
        steps = jax.random.uniform(jax.random.fold_in(jax.random.fold_in(key, 6), dim), (parts,), jnp.float32, low / len(cuts), top_value / len(cuts))
        return jnp.repeat(jnp.exp(steps), dims[dim] // parts).reshape((-1,) + (1,) * (len(dims) - dim - 1))

    loudness = one(*cuts[0])
    for cut in cuts[1:]:
        loudness = loudness * one(*cut)
    return loudness


def normal_values(key, shape, deviation, reach, shards=(), kind=jnp.bfloat16):
    entries = jax.random.normal(key, shape, jnp.float32) * deviation
    if len(shards) > 0:
        entries = levels(key, shape, shards, -0.22, 0.18) * entries
    return jnp.clip(entries, min=-reach, max=reach).astype(kind)


def setup_inputs(seed: int = 0) -> dict:
    arg_keys = jax.random.split(jax.random.key(seed), 8)
    return {
        "tokens": normal_values(arg_keys[0], (SEQ, D), 1.0, 6.0, ((0, 8), (1, 4))),
        "in_proj": normal_values(arg_keys[1], (LAYERS, D, P_SIZE), D ** -0.5, 0.09375, ((1, 4), (2, 8))),
        "group_mix": normal_values(arg_keys[2], (LAYERS, 4, POOL_CH, POOL_CH), POOL_CH ** -0.5, 0.375),
        "pool_gain": jnp.clip(1.0 + 0.18 * jax.random.normal(arg_keys[3], (LAYERS, P_SIZE), jnp.float32), 0.1, 1.9),
        "out_proj": normal_values(arg_keys[4], (LAYERS, P_SIZE, D), P_SIZE ** -0.5, 0.1875, ((1, 8), (2, 4))),
        "norm_gain": draw_norm_gain(jax.random.fold_in(arg_keys[7], 71), 0),
        "norm_bias": normal_values(arg_keys[6], (LAYERS, D), 0.3, 1.5, ((1, 4),), jnp.float32),
    }


pool_windows = (2, 4, 8, 16)
norm_eps = 1e-05

def reference(tokens, in_proj, group_mix, pool_gain, out_proj, norm_gain, norm_bias):
    residual_scale = (2.0 * LAYERS) ** 0.25
    stream = tokens
    seq_length = stream.shape[0]
    positions = jnp.arange(seq_length)
    block_width = D // N_TP
    fringe_width = max(pool_windows) // 2
    for layer_idx in range(LAYERS):
        summed = jnp.zeros((seq_length, P_SIZE), jnp.float32)
        for block_idx in range(N_TP):
            first_col = block_idx * block_width
            partial_term = jnp.dot(stream[:, first_col:first_col + block_width], in_proj[layer_idx, first_col:first_col + block_width], preferred_element_type=jnp.float32).astype(jnp.bfloat16)
            summed = summed + partial_term.astype(jnp.float32)
        projected = summed.astype(jnp.bfloat16)
        proj_float = projected.astype(jnp.float32)
        padded = jnp.pad(proj_float, ((fringe_width, fringe_width), (0, 0)))
        mixed_parts = []
        for group_idx in range(4):
            span_len = pool_windows[group_idx]
            before = span_len // 2
            after = span_len - before
            group_cols = slice(group_idx * POOL_CH, (group_idx + 1) * POOL_CH)
            window_total = jnp.zeros((seq_length, POOL_CH), jnp.float32)
            for offset in range(-before, after):
                window_total = window_total + padded[fringe_width + offset:fringe_width + offset + seq_length, group_cols]
            low_edge = jnp.clip(positions - before, 0, seq_length)
            high_edge = jnp.clip(positions + after, 0, seq_length)
            pooled = window_total / (high_edge - low_edge).astype(jnp.float32)[:, None]
            differ = (pooled - proj_float[:, group_cols]).astype(jnp.bfloat16)
            mixed_parts.append(jnp.dot(differ, group_mix[layer_idx, group_idx], preferred_element_type=jnp.float32))
        mixed_out = (jnp.concatenate(mixed_parts, axis=1) * pool_gain[layer_idx][None, :]).astype(jnp.bfloat16)
        branch = jnp.dot(mixed_out, out_proj[layer_idx], preferred_element_type=jnp.float32)
        resid = residual_scale * stream.astype(jnp.float32) + branch
        row_mean = lax.optimization_barrier(jnp.mean(resid, axis=1, keepdims=True))
        row_var = lax.optimization_barrier(jnp.mean(jnp.square(resid - row_mean), axis=1, keepdims=True))
        normed = (resid - row_mean) * lax.rsqrt(row_var + norm_eps)
        stream = (normed * norm_gain[layer_idx][None, :] + norm_bias[layer_idx][None, :]).astype(jnp.bfloat16)
    return stream
```

```python
import functools

import jax
import jax.numpy as jnp
from jax import lax
from jax.experimental import pallas as pl
from jax.experimental.pallas import tpu as pltpu
from jax.sharding import PartitionSpec as P

MESH = pl.DeviceIdType.MESH
F32 = jnp.float32
BF16 = jnp.bfloat16

pool_windows = (2, 4, 8, 16)
norm_eps = 1e-05


def padded(array, sides, width):
    for axis, dim in sides:
        devices, length = (lax.axis_size(axis), array.shape[dim])
        up = [(i, (i + 1) % devices) for i in range(devices - 1)]
        down = [(j, i) for i, j in up]
        last = lax.slice_in_dim(array, length - width, length, axis=dim)
        leading = lax.slice_in_dim(array, 0, width, axis=dim)
        before = lax.ppermute(last, axis, up)
        after = lax.ppermute(leading, axis, down)
        array = jnp.concatenate([before, array, after], axis=dim)
    return array


def on_device(tokens, in_proj, group_mix, pool_gain, out_proj, norm_gain, norm_bias):
    rows_dev = tokens.shape[0]
    feat_dev = tokens.shape[1]
    layer_count = in_proj.shape[0]
    pool_width = in_proj.shape[2] * lax.axis_size("sp")
    chan_share = pool_width // lax.axis_size("tp")
    group_width = group_mix.shape[2]
    model_width = feat_dev * lax.axis_size("tp")
    residual_scale = (2.0 * layer_count) ** 0.25
    fringe_width = max(pool_windows) // 2
    seq_length = rows_dev * lax.axis_size("sp")
    positions = lax.axis_index("sp") * rows_dev + jnp.arange(rows_dev)
    chan_groups = (lax.axis_index("tp") * chan_share + jnp.arange(chan_share)) // group_width
    in_all, out_all = (
        lax.all_gather(in_proj, "sp", axis=2, tiled=True),
        lax.all_gather(out_proj, "sp", axis=1, tiled=True),
    )
    stream = tokens
    for layer_idx in range(layer_count):
        in_block = in_all[layer_idx]
        out_block = out_all[layer_idx]
        projected = lax.psum_scatter(
            lax.dot_general(
                in_block, stream, (((0,), (1,)), ((), ())), preferred_element_type=jnp.float32
            ).astype(jnp.bfloat16),
            "tp",
            scatter_dimension=0,
            tiled=True,
        )
        extended = padded(projected, (("sp", 1),), fringe_width)
        ext_float = extended.astype(jnp.float32)
        pooled = jnp.zeros((chan_share, rows_dev), jnp.float32)
        for group_idx in range(4):
            own_rows = (chan_groups == group_idx)[:, None]
            span_len = pool_windows[group_idx]
            before = span_len // 2
            after = span_len - before
            window_total = jnp.zeros((ext_float.shape[0], rows_dev), jnp.float32)
            for offset in range(-before, after):
                window_total = (
                    window_total
                    + ext_float[:, fringe_width + offset : fringe_width + offset + rows_dev]
                )
            low_edge = jnp.clip(positions - before, 0, seq_length)
            high_edge = jnp.clip(positions + after, 0, seq_length)
            pooled = jnp.where(
                own_rows, window_total / (high_edge - low_edge).astype(jnp.float32)[None, :], pooled
            )
        differ = (pooled - projected.astype(jnp.float32)).astype(jnp.bfloat16)
        all_differ = lax.all_gather(differ, "tp", axis=0, tiled=True)
        grouped = all_differ.reshape(4, group_width, rows_dev)
        mixed_all = jnp.einsum(
            "gcd,gct->gdt", group_mix[layer_idx], grouped, preferred_element_type=jnp.float32
        ).reshape(pool_width, rows_dev)
        mixed_all = (mixed_all * pool_gain[layer_idx][:, None]).astype(jnp.bfloat16)
        branch = lax.dot_general(
            mixed_all, out_block, (((0,), (0,)), ((), ())), preferred_element_type=jnp.float32
        )
        resid = residual_scale * stream.astype(jnp.float32) + branch
        row_sums, squares = lax.psum((jnp.sum(resid, axis=1), jnp.sum(resid * resid, axis=1)), "tp")
        row_mean = row_sums / model_width
        row_var = squares / model_width - row_mean * row_mean
        normed = (resid - row_mean[:, None]) * lax.rsqrt(row_var[:, None] + norm_eps)
        stream = (normed * norm_gain[layer_idx][None, :] + norm_bias[layer_idx][None, :]).astype(
            jnp.bfloat16
        )
    return stream


def mixer_kernel(
    cfg,
    tok,
    win,
    mixw,
    gain,
    wout,
    ngain,
    nbias,
    out,
    in_all,
    out_all,
    strm,
    part_send,
    part_recv,
    px_send,
    px_recv,
    ext,
    mix_all,
    resid,
    lanes,
    stat_send,
    stat_recv,
    mean_col,
    rstd_col,
    wsend,
    wrecv,
    hsend,
    hrecv,
    asend,
    arecv,
):
    n_sp, n_tp, ydim, halo = cfg
    zdim = n_sp // ydim
    layers = win.shape[0]
    rows_dev, feat = tok.shape
    rows = strm.shape[0]
    pad = max(pool_windows) // 2
    gw = mixw.shape[1]
    cw = win.shape[2]
    ow = wout.shape[1]
    seq = rows_dev * n_sp
    model = feat * n_tp
    alpha = (2.0 * layers) ** 0.25
    big = rows // 2
    small = rows // 4
    out_tile = rows_dev // 4
    me_sp = lax.axis_index("sp")
    me = lax.axis_index("tp")
    z = me_sp // ydim
    y = me_sp % ydim
    ypeer = z * ydim + (ydim - 1 - y)
    core = me % 2
    xid = me // 2
    sib = xid * 2 + (1 - core)
    xo = (1 - xid) * 2 + core

    barrier = pltpu.get_barrier_semaphore()
    for d in range(1, n_sp):
        pl.semaphore_signal(barrier, inc=1, device_id=((me_sp + d) % n_sp, me), device_id_type=MESH)
    for d in range(1, n_tp):
        pl.semaphore_signal(barrier, inc=1, device_id=(me_sp, (me + d) % n_tp), device_id_type=MESH)
    pl.semaphore_wait(barrier, n_sp + n_tp - 2)

    def remote(src, dst, ssem, rsem, dev):
        return pltpu.make_async_remote_copy(
            src_ref=src, dst_ref=dst, send_sem=ssem, recv_sem=rsem, device_id=dev, device_id_type=MESH
        )

    def halo_up():
        return remote(
            tok.at[pl.ds(rows_dev - halo, halo)], strm.at[pl.ds(0, halo)],
            hsend.at[0], hrecv.at[0], ((me_sp + 1) % n_sp, me),
        )

    def halo_down():
        return remote(
            tok.at[pl.ds(0, halo)], strm.at[pl.ds(halo + rows_dev, halo)],
            hsend.at[1], hrecv.at[1], ((me_sp + n_sp - 1) % n_sp, me),
        )

    @pl.when(me_sp < n_sp - 1)
    def _():
        halo_up().start()

    @pl.when(me_sp > 0)
    def _():
        halo_down().start()

    def shard(b, s):
        l = b // 2
        if b % 2 == 0:
            return in_all.at[l, :, pl.ds(pl.multiple_of(s * cw, cw), cw)]
        return out_all.at[l, pl.ds(pl.multiple_of(s * ow, ow), ow), :]

    def own(b):
        return win.at[b // 2] if b % 2 == 0 else wout.at[b // 2]

    def wy(b):
        return remote(own(b), shard(b, me_sp), wsend.at[b, 0], wrecv.at[b, me_sp], (ypeer, me))

    def wz(b, d):
        dev = ((z + d) % zdim) * ydim + y
        return remote(own(b), shard(b, me_sp), wsend.at[b, d], wrecv.at[b, me_sp], (dev, me))

    def wrelay(b, d):
        s = ((z + d) % zdim) * ydim + y
        return remote(shard(b, s), shard(b, s), wsend.at[b, zdim - 1 + d], wrecv.at[b, s], (ypeer, me))

    def issue(b):
        wy(b).start()
        for d in range(1, zdim):
            wz(b, d).start()

    def relay(b):
        for d in range(1, zdim):
            copy = wrelay(b, d)
            copy.wait_recv()
            copy.start()

    def finish(b):
        for d in range(zdim):
            s = ((z + d) % zdim) * ydim + (ydim - 1 - y)
            remote(shard(b, s), shard(b, s), wsend.at[b, 0], wrecv.at[b, s], (ypeer, me)).wait_recv()

    blocks = 2 * layers
    issue(0)
    issue(1)

    for l in range(layers):
        in_all[l, :, pl.ds(pl.multiple_of(me_sp * cw, cw), cw)] = win[l]
        out_all[l, pl.ds(pl.multiple_of(me_sp * ow, ow), ow), :] = wout[l]
    strm[pl.ds(halo, rows_dev), :] = tok[...]

    @pl.when(me_sp == 0)
    def _():
        strm[pl.ds(0, halo), :] = jnp.zeros((halo, feat), BF16)

    @pl.when(me_sp == n_sp - 1)
    def _():
        strm[pl.ds(halo + rows_dev, halo), :] = jnp.zeros((halo, feat), BF16)

    ext[pl.ds(0, pad), :] = jnp.zeros((pad, gw), F32)
    ext[pl.ds(pad + rows, pad), :] = jnp.zeros((pad, gw), F32)
    lanes[...] = jnp.zeros(lanes.shape, F32)
    stat_send[...] = jnp.zeros(stat_send.shape, F32)
    sb = lanes.shape[1] // 128

    @pl.when(me_sp > 0)
    def _():
        halo_up().wait_recv()

    @pl.when(me_sp < n_sp - 1)
    def _():
        halo_down().wait_recv()

    def loop(count, body):
        lax.fori_loop(0, count, lambda i, c: (body(i), c)[1], 0)

    for l in range(layers):
        relay(2 * l)
        if 2 * l + 2 < blocks:
            issue(2 * l + 2)
        finish(2 * l)

        def in_dot(r, g):
            return jnp.dot(
                strm[r, :],
                in_all[l, :, pl.ds(pl.multiple_of(g * gw, gw), gw)],
                preferred_element_type=F32,
            )

        def body1(i):
            r = pl.ds(pl.multiple_of(i * big, 16), big)
            for q in range(2):
                part_send[q, r, :] = in_dot(r, q * 2 + (1 - core)).astype(BF16)

        loop(2, body1)
        cpart = remote(part_send, part_recv, asend.at[0], arecv.at[0], (me_sp, sib))
        cpart.start()

        def body2(i):
            r = pl.ds(pl.multiple_of(i * big, 16), big)
            resid[r, pl.ds(0, gw)] = in_dot(r, xo)
            resid[r, pl.ds(gw, gw)] = in_dot(r, me)

        loop(2, body2)
        cpart.wait_recv()

        def body3(i):
            r = pl.ds(pl.multiple_of(i * small, 16), small)
            px_send[r, :] = (resid[r, pl.ds(0, gw)] + part_recv[1 - xid, r, :].astype(F32)).astype(BF16)

        loop(4, body3)
        cpx = remote(px_send, px_recv, asend.at[1], arecv.at[1], (me_sp, xo))
        cpx.start()

        def body4(i):
            r = pl.ds(pl.multiple_of(i * small, 16), small)
            resid[r, pl.ds(gw, gw)] = resid[r, pl.ds(gw, gw)] + part_recv[xid, r, :].astype(F32)

        loop(4, body4)
        cpx.wait_recv()

        def body5(i):
            r = pl.ds(pl.multiple_of(i * small, 16), small)
            total = resid[r, pl.ds(gw, gw)] + px_recv[r, :].astype(F32)
            proj = total.astype(BF16).astype(F32)
            pos = lax.broadcasted_iota(jnp.int32, (small, gw), 0) + (me_sp * rows_dev - halo + i * small)
            proj = jnp.where((pos >= 0) & (pos < seq), proj, 0.0)
            ext[pl.ds(pl.multiple_of(pad + i * small, 8), small), :] = proj

        loop(4, body5)

        def body6(i):
            n = small + 2 * pad
            v = ext[pl.ds(pl.multiple_of(i * small, 8), n), :]
            w = v + pltpu.roll(v, 1, 0)
            window = w
            half = 1
            for g in range(1, len(pool_windows)):
                w = pltpu.roll(w, half, 0) + pltpu.roll(w, n - half, 0)
                window = jnp.where(me == g, w, window)
                half *= 2
            span = jnp.left_shift(1, me)
            pos = lax.broadcasted_iota(jnp.int32, (small, gw), 0) + (me_sp * rows_dev - halo + i * small)
            count = jnp.minimum(pos + span, seq) - jnp.maximum(pos - span, 0)
            count = jnp.maximum(count, 1).astype(F32)
            differ = (window[pad : pad + small] / count - v[pad : pad + small]).astype(BF16)
            mixed = jnp.dot(differ, mixw[l], preferred_element_type=F32) * gain[l]
            r = pl.ds(pl.multiple_of(i * small, 16), small)
            mix_all[r, pl.ds(pl.multiple_of(me * gw, gw), gw)] = mixed.astype(BF16)

        loop(4, body6)

        def msl(g):
            return mix_all.at[:, pl.ds(pl.multiple_of(g * gw, gw), gw)]

        c_x = remote(msl(me), msl(me), asend.at[2], arecv.at[2], (me_sp, xo))
        c_s = remote(msl(me), msl(me), asend.at[3], arecv.at[3], (me_sp, sib))
        c_x.start()
        c_s.start()
        relay(2 * l + 1)
        if 2 * l + 3 < blocks:
            issue(2 * l + 3)
        c_r = remote(msl(xo), msl(xo), asend.at[4], arecv.at[4], (me_sp, sib))
        remote(msl(xo), msl(xo), asend.at[2], arecv.at[2], (me_sp, xo)).wait_recv()
        c_r.start()
        finish(2 * l + 1)
        remote(msl(sib), msl(sib), asend.at[3], arecv.at[3], (me_sp, sib)).wait_recv()
        dia = (1 - xid) * 2 + (1 - core)
        remote(msl(dia), msl(dia), asend.at[4], arecv.at[4], (me_sp, sib)).wait_recv()

        def body7(i):
            r = pl.ds(pl.multiple_of(i * small, 16), small)
            branch = jnp.dot(mix_all[r, :], out_all[l], preferred_element_type=F32)
            res = alpha * strm[r, :].astype(F32) + branch
            resid[r, :] = res
            sq = res * res
            a = res[:, 0:128]
            b = sq[:, 0:128]
            for k in range(1, feat // 128):
                a = a + res[:, k * 128 : (k + 1) * 128]
                b = b + sq[:, k * 128 : (k + 1) * 128]
            lanes[0, r, :] = a
            lanes[1, r, :] = b

        loop(4, body7)
        for k in range(sb):
            for q in range(2):
                blk = lanes[q, k * 128 : (k + 1) * 128, :]
                stat_send[k : k + 1, q * 128 : (q + 1) * 128] = jnp.sum(blk.T, axis=0, keepdims=True)
        stats = []
        for d in range(1, n_tp):
            c = remote(
                stat_send, stat_recv.at[d - 1], asend.at[4 + d], arecv.at[4 + d], (me_sp, (me + d) % n_tp)
            )
            c.start()
            stats.append(c)
        for c in stats:
            c.wait_recv()
        total = stat_send[...]
        for d in range(1, n_tp):
            total = total + stat_recv[d - 1]
        mean = total[:, 0:128] / model
        var = total[:, 128:256] / model - mean * mean
        rstd = lax.rsqrt(var + norm_eps)
        for k in range(sb):
            mean_col[k * 128 : (k + 1) * 128, :] = jnp.broadcast_to(mean[k : k + 1, :], (128, 128)).T
            rstd_col[k * 128 : (k + 1) * 128, :] = jnp.broadcast_to(rstd[k : k + 1, :], (128, 128)).T

        def normed(r, k):
            ks = pl.ds(k * 128, 128)
            t = (resid[r, ks] - mean_col[r, :]) * rstd_col[r, :]
            return (t * ngain[l, :, ks] + nbias[l, :, ks]).astype(BF16)

        last = l == layers - 1

        def body8(i):
            if last:
                r = pl.ds(pl.multiple_of(halo + i * out_tile, 16), out_tile)
                o = pl.ds(pl.multiple_of(i * out_tile, 16), out_tile)
            else:
                r = pl.ds(pl.multiple_of(i * small, 16), small)
            for k in range(feat // 128):
                if last:
                    out[o, pl.ds(k * 128, 128)] = normed(r, k)
                else:
                    strm[r, pl.ds(k * 128, 128)] = normed(r, k)

        loop(4, body8)
        for c in [cpart, cpx, c_x, c_s, c_r] + stats:
            c.wait_send()

    @pl.when(me_sp < n_sp - 1)
    def _():
        halo_up().wait_send()

    @pl.when(me_sp > 0)
    def _():
        halo_down().wait_send()

    for b in range(blocks):
        wy(b).wait_send()
        for d in range(1, zdim):
            wz(b, d).wait_send()
            wrelay(b, d).wait_send()


def in_one_kernel(n_sp, n_tp, tokens, in_proj, group_mix, pool_gain, out_proj, norm_gain, norm_bias):
    rows_dev, feat = tokens.shape
    layers = in_proj.shape[0]
    gw = group_mix.shape[2]
    width = in_proj.shape[2] * n_sp
    ydim = 2
    halo = -(-layers * (max(pool_windows) // 2) // 32) * 32
    rows = rows_dev + 2 * halo
    rows_pad = -(-rows // 128) * 128
    me = lax.axis_index("tp")
    mixw = lax.dynamic_index_in_dim(group_mix, me, axis=1, keepdims=False)
    gain = lax.dynamic_slice_in_dim(pool_gain, me * gw, gw, axis=1)[:, None, :]
    pad = max(pool_windows) // 2
    vmem = pl.BlockSpec(memory_space=pltpu.VMEM)
    zdim = n_sp // ydim
    blocks = 2 * layers
    return pl.pallas_call(
        functools.partial(mixer_kernel, (n_sp, n_tp, ydim, halo)),
        out_shape=jax.ShapeDtypeStruct((rows_dev, feat), BF16),
        in_specs=[vmem] * 7,
        out_specs=vmem,
        scratch_shapes=[
            pltpu.VMEM((layers, feat, width), BF16),
            pltpu.VMEM((layers, width, feat), BF16),
            pltpu.VMEM((rows, feat), BF16),
            pltpu.VMEM((2, rows, gw), BF16),
            pltpu.VMEM((2, rows, gw), BF16),
            pltpu.VMEM((rows, gw), BF16),
            pltpu.VMEM((rows, gw), BF16),
            pltpu.VMEM((rows + 2 * pad, gw), F32),
            pltpu.VMEM((rows, width), BF16),
            pltpu.VMEM((rows, feat), F32),
            pltpu.VMEM((2, rows_pad, 128), F32),
            pltpu.VMEM((-(-rows_pad // 1024) * 8, 256), F32),
            pltpu.VMEM((n_tp - 1, -(-rows_pad // 1024) * 8, 256), F32),
            pltpu.VMEM((rows_pad, 128), F32),
            pltpu.VMEM((rows_pad, 128), F32),
            pltpu.SemaphoreType.DMA((blocks, 2 * zdim - 1)),
            pltpu.SemaphoreType.DMA((blocks, n_sp)),
            pltpu.SemaphoreType.DMA((2,)),
            pltpu.SemaphoreType.DMA((2,)),
            pltpu.SemaphoreType.DMA((4 + n_tp,)),
            pltpu.SemaphoreType.DMA((4 + n_tp,)),
        ],
        compiler_params=pltpu.CompilerParams(
            collective_id=0, has_side_effects=True, vmem_limit_bytes=60 * 1024 * 1024
        ),
    )(tokens, in_proj, mixw, gain, out_proj, norm_gain[:, None, :], norm_bias[:, None, :])


def one_kernel_fits(n_sp, n_tp, tokens, in_proj, group_mix):
    rows_dev = tokens.shape[0] // n_sp
    return (
        n_tp == 4
        and group_mix.shape[1] == n_tp
        and in_proj.shape[2] == n_tp * group_mix.shape[2]
        and group_mix.shape[2] % 128 == 0
        and n_sp % 2 == 0
        and (in_proj.shape[2] // n_sp) % 128 == 0
        and rows_dev % 64 == 0
        and (tokens.shape[1] // n_tp) % 128 == 0
    )


def solution(mesh):
    in_specs = (
        P("sp", "tp"),
        P(None, "tp", "sp"),
        P(),
        P(),
        P(None, "sp", "tp"),
        P(None, "tp"),
        P(None, "tp"),
    )
    out_specs = P("sp", "tp")
    n_sp, n_tp = mesh.shape["sp"], mesh.shape["tp"]

    def run(tokens, in_proj, group_mix, *rest):
        body = on_device
        if one_kernel_fits(n_sp, n_tp, tokens, in_proj, group_mix):
            body = functools.partial(in_one_kernel, n_sp, n_tp)
        return jax.shard_map(
            body, mesh=mesh, in_specs=in_specs, out_specs=out_specs, check_vma=False
        )(tokens, in_proj, group_mix, *rest)

    return run
```

```python
import functools

import jax
import jax.numpy as jnp
from jax import lax
from jax.experimental import pallas as pl
from jax.experimental.pallas import tpu as pltpu
from jax.sharding import PartitionSpec as P

MESH = pl.DeviceIdType.MESH
F32 = jnp.float32
BF16 = jnp.bfloat16

pool_windows = (2, 4, 8, 16)
norm_eps = 1e-05


def padded(array, sides, width):
    for axis, dim in sides:
        devices, length = (lax.axis_size(axis), array.shape[dim])
        up = [(i, (i + 1) % devices) for i in range(devices - 1)]
        down = [(j, i) for i, j in up]
        last = lax.slice_in_dim(array, length - width, length, axis=dim)
        leading = lax.slice_in_dim(array, 0, width, axis=dim)
        before = lax.ppermute(last, axis, up)
        after = lax.ppermute(leading, axis, down)
        array = jnp.concatenate([before, array, after], axis=dim)
    return array


def on_device(tokens, in_proj, group_mix, pool_gain, out_proj, norm_gain, norm_bias):
    rows_dev = tokens.shape[0]
    feat_dev = tokens.shape[1]
    layer_count = in_proj.shape[0]
    pool_width = in_proj.shape[2] * lax.axis_size("sp")
    chan_share = pool_width // lax.axis_size("tp")
    group_width = group_mix.shape[2]
    model_width = feat_dev * lax.axis_size("tp")
    residual_scale = (2.0 * layer_count) ** 0.25
    fringe_width = max(pool_windows) // 2
    seq_length = rows_dev * lax.axis_size("sp")
    positions = lax.axis_index("sp") * rows_dev + jnp.arange(rows_dev)
    chan_groups = (lax.axis_index("tp") * chan_share + jnp.arange(chan_share)) // group_width
    in_all, out_all = (
        lax.all_gather(in_proj, "sp", axis=2, tiled=True),
        lax.all_gather(out_proj, "sp", axis=1, tiled=True),
    )
    stream = tokens
    for layer_idx in range(layer_count):
        in_block = in_all[layer_idx]
        out_block = out_all[layer_idx]
        projected = lax.psum_scatter(
            lax.dot_general(
                in_block, stream, (((0,), (1,)), ((), ())), preferred_element_type=jnp.float32
            ).astype(jnp.bfloat16),
            "tp",
            scatter_dimension=0,
            tiled=True,
        )
        extended = padded(projected, (("sp", 1),), fringe_width)
        ext_float = extended.astype(jnp.float32)
        pooled = jnp.zeros((chan_share, rows_dev), jnp.float32)
        for group_idx in range(4):
            own_rows = (chan_groups == group_idx)[:, None]
            span_len = pool_windows[group_idx]
            before = span_len // 2
            after = span_len - before
            window_total = jnp.zeros((ext_float.shape[0], rows_dev), jnp.float32)
            for offset in range(-before, after):
                window_total = (
                    window_total
                    + ext_float[:, fringe_width + offset : fringe_width + offset + rows_dev]
                )
            low_edge = jnp.clip(positions - before, 0, seq_length)
            high_edge = jnp.clip(positions + after, 0, seq_length)
            pooled = jnp.where(
                own_rows, window_total / (high_edge - low_edge).astype(jnp.float32)[None, :], pooled
            )
        differ = (pooled - projected.astype(jnp.float32)).astype(jnp.bfloat16)
        all_differ = lax.all_gather(differ, "tp", axis=0, tiled=True)
        grouped = all_differ.reshape(4, group_width, rows_dev)
        mixed_all = jnp.einsum(
            "gcd,gct->gdt", group_mix[layer_idx], grouped, preferred_element_type=jnp.float32
        ).reshape(pool_width, rows_dev)
        mixed_all = (mixed_all * pool_gain[layer_idx][:, None]).astype(jnp.bfloat16)
        branch = lax.dot_general(
            mixed_all, out_block, (((0,), (0,)), ((), ())), preferred_element_type=jnp.float32
        )
        resid = residual_scale * stream.astype(jnp.float32) + branch
        row_sums, squares = lax.psum((jnp.sum(resid, axis=1), jnp.sum(resid * resid, axis=1)), "tp")
        row_mean = row_sums / model_width
        row_var = squares / model_width - row_mean * row_mean
        normed = (resid - row_mean[:, None]) * lax.rsqrt(row_var[:, None] + norm_eps)
        stream = (normed * norm_gain[layer_idx][None, :] + norm_bias[layer_idx][None, :]).astype(
            jnp.bfloat16
        )
    return stream


def mixer_kernel(
    cfg,
    tok,
    win,
    mixw,
    gain,
    wout,
    ngain,
    nbias,
    out,
    in_all,
    out_all,
    strm,
    part_send,
    part_recv,
    px_send,
    px_recv,
    ext,
    mix_all,
    resid,
    lanes,
    stat_send,
    stat_recv,
    mean_col,
    rstd_col,
    wsend,
    wrecv,
    hsend,
    hrecv,
    asend,
    arecv,
):
    n_sp, n_tp, ydim, halo = cfg
    zdim = n_sp // ydim
    layers = win.shape[0]
    rows_dev, feat = tok.shape
    rows = strm.shape[0]
    pad = max(pool_windows) // 2
    gw = mixw.shape[1]
    cw = win.shape[2]
    ow = wout.shape[1]
    seq = rows_dev * n_sp
    model = feat * n_tp
    alpha = (2.0 * layers) ** 0.25
    big = rows // 2
    small = rows // 4
    out_tile = rows_dev // 4
    me_sp = lax.axis_index("sp")
    me = lax.axis_index("tp")
    z = me_sp // ydim
    y = me_sp % ydim
    ypeer = z * ydim + (ydim - 1 - y)
    core = me % 2
    xid = me // 2
    sib = xid * 2 + (1 - core)
    xo = (1 - xid) * 2 + core

    barrier = pltpu.get_barrier_semaphore()
    for d in range(1, n_sp):
        pl.semaphore_signal(barrier, inc=1, device_id=((me_sp + d) % n_sp, me), device_id_type=MESH)
    for d in range(1, n_tp):
        pl.semaphore_signal(barrier, inc=1, device_id=(me_sp, (me + d) % n_tp), device_id_type=MESH)
    pl.semaphore_wait(barrier, n_sp + n_tp - 2)

    def remote(src, dst, ssem, rsem, dev):
        return pltpu.make_async_remote_copy(
            src_ref=src, dst_ref=dst, send_sem=ssem, recv_sem=rsem, device_id=dev, device_id_type=MESH
        )

    def halo_up():
        return remote(
            tok.at[pl.ds(rows_dev - halo, halo)], strm.at[pl.ds(0, halo)],
            hsend.at[0], hrecv.at[0], ((me_sp + 1) % n_sp, me),
        )

    def halo_down():
        return remote(
            tok.at[pl.ds(0, halo)], strm.at[pl.ds(halo + rows_dev, halo)],
            hsend.at[1], hrecv.at[1], ((me_sp + n_sp - 1) % n_sp, me),
        )

    @pl.when(me_sp < n_sp - 1)
    def _():
        halo_up().start()

    @pl.when(me_sp > 0)
    def _():
        halo_down().start()

    def shard(b, s):
        l = b // 2
        if b % 2 == 0:
            return in_all.at[l, :, pl.ds(pl.multiple_of(s * cw, cw), cw)]
        return out_all.at[l, pl.ds(pl.multiple_of(s * ow, ow), ow), :]

    def own(b):
        return win.at[b // 2] if b % 2 == 0 else wout.at[b // 2]

    yf_block = -1
    blocks = 2 * layers
    top = z < zdim - 1
    low = z > 0

    def fwd(b, s, src, kind):
        dev = (ypeer, (me_sp + ydim) % n_sp, (me_sp + n_sp - ydim) % n_sp)[kind]
        return remote(src, shard(b, s), wsend.at[b, kind, s], wrecv.at[b, s], (dev, me))

    def arrived(b, s):
        fwd(b, s, shard(b, s), 0).wait_recv()

    def send(b, s, src, kind, cond=None):
        if cond is None:
            fwd(b, s, src, kind).start()
        else:

            @pl.when(cond)
            def _():
                fwd(b, s, src, kind).start()

    def issue(b):
        send(b, me_sp, own(b), 1, top)
        send(b, me_sp, own(b), 2, low)
        send(b, me_sp, own(b), 0)

    def step(b, k):
        if k == 0:
            s0 = ypeer
            arrived(b, s0)
            send(b, s0, shard(b, s0), 1, top)
            send(b, s0, shard(b, s0), 2, low)
            return
        yf = b == yf_block
        for base in (me_sp, ypeer) if yf else (me_sp,):

            @pl.when(z >= k)
            def _():
                sb = base - k * ydim
                arrived(b, sb)
                send(b, sb, shard(b, sb), 1, top)
                if not yf:
                    send(b, sb, shard(b, sb), 0)

            @pl.when(z + k < zdim)
            def _():
                sa = base + k * ydim
                arrived(b, sa)
                send(b, sa, shard(b, sa), 2, low)
                if not yf:
                    send(b, sa, shard(b, sa), 0)

    def finish(b):
        if b != yf_block:
            for d in range(zdim):
                arrived(b, ((z + d) % zdim) * ydim + (ydim - 1 - y))

    def drain(b):
        yf = b == yf_block
        fwd(b, me_sp, own(b), 0).wait_send()
        for k in range(zdim):
            if k > 0 and not yf:
                s = ((z + k) % zdim) * ydim + y
                fwd(b, s, shard(b, s), 0).wait_send()
            for base in (me_sp, ypeer) if yf else (me_sp,):

                @pl.when((z >= k) & top)
                def _():
                    sb = base - k * ydim
                    fwd(b, sb, shard(b, sb), 1).wait_send()

                @pl.when((z + k < zdim) & low)
                def _():
                    sa = base + k * ydim
                    fwd(b, sa, shard(b, sa), 2).wait_send()

    events = [(b, k) for b in range(blocks) for k in range(0 if b == yf_block else 1, zdim)]
    ahead = 3

    def pump(count):
        for _ in range(min(count, len(events))):
            b, k = events.pop(0)
            step(b, k)
            if k == zdim - 1 and b + ahead < blocks:
                issue(b + ahead)

    def need(b):
        while events and events[0][0] <= b:
            pump(1)
        finish(b)

    for b in range(min(ahead, blocks)):
        issue(b)

    for l in range(layers):
        in_all[l, :, pl.ds(pl.multiple_of(me_sp * cw, cw), cw)] = win[l]
        out_all[l, pl.ds(pl.multiple_of(me_sp * ow, ow), ow), :] = wout[l]
    strm[pl.ds(halo, rows_dev), :] = tok[...]

    @pl.when(me_sp == 0)
    def _():
        strm[pl.ds(0, halo), :] = jnp.zeros((halo, feat), BF16)

    @pl.when(me_sp == n_sp - 1)
    def _():
        strm[pl.ds(halo + rows_dev, halo), :] = jnp.zeros((halo, feat), BF16)

    ext[pl.ds(0, pad), :] = jnp.zeros((pad, gw), F32)
    ext[pl.ds(pad + rows, pad), :] = jnp.zeros((pad, gw), F32)
    lanes[...] = jnp.zeros(lanes.shape, F32)
    stat_send[...] = jnp.zeros(stat_send.shape, F32)
    sb = lanes.shape[1] // 128

    @pl.when(me_sp > 0)
    def _():
        halo_up().wait_recv()

    @pl.when(me_sp < n_sp - 1)
    def _():
        halo_down().wait_recv()

    def loop(count, body):
        lax.fori_loop(0, count, lambda i, c: (body(i), c)[1], 0)

    for l in range(layers):
        need(2 * l)

        def in_dot(r, g):
            return jnp.dot(
                strm[r, :],
                in_all[l, :, pl.ds(pl.multiple_of(g * gw, gw), gw)],
                preferred_element_type=F32,
            )

        def body1(i):
            r = pl.ds(pl.multiple_of(i * big, 16), big)
            for q in range(2):
                part_send[q, r, :] = in_dot(r, q * 2 + (1 - core)).astype(BF16)

        loop(2, body1)
        cpart = remote(part_send, part_recv, asend.at[0], arecv.at[0], (me_sp, sib))
        cpart.start()
        pump(1)

        def body2(i):
            r = pl.ds(pl.multiple_of(i * big, 16), big)
            resid[r, pl.ds(0, gw)] = in_dot(r, xo)
            resid[r, pl.ds(gw, gw)] = in_dot(r, me)

        loop(2, body2)
        cpart.wait_recv()

        def body3(i):
            r = pl.ds(pl.multiple_of(i * small, 16), small)
            px_send[r, :] = (resid[r, pl.ds(0, gw)] + part_recv[1 - xid, r, :].astype(F32)).astype(BF16)

        loop(4, body3)
        cpx = remote(px_send, px_recv, asend.at[1], arecv.at[1], (me_sp, xo))
        cpx.start()
        pump(2)

        def body4(i):
            r = pl.ds(pl.multiple_of(i * small, 16), small)
            resid[r, pl.ds(gw, gw)] = resid[r, pl.ds(gw, gw)] + part_recv[xid, r, :].astype(F32)

        loop(4, body4)
        pump(2)
        cpx.wait_recv()

        def body5(i):
            r = pl.ds(pl.multiple_of(i * small, 16), small)
            total = resid[r, pl.ds(gw, gw)] + px_recv[r, :].astype(F32)
            proj = total.astype(BF16).astype(F32)
            pos = lax.broadcasted_iota(jnp.int32, (small, gw), 0) + (me_sp * rows_dev - halo + i * small)
            proj = jnp.where((pos >= 0) & (pos < seq), proj, 0.0)
            ext[pl.ds(pl.multiple_of(pad + i * small, 8), small), :] = proj

        loop(4, body5)

        def body6(i):
            n = small + 2 * pad
            v = ext[pl.ds(pl.multiple_of(i * small, 8), n), :]
            w = v + pltpu.roll(v, 1, 0)
            window = w
            half = 1
            for g in range(1, len(pool_windows)):
                w = pltpu.roll(w, half, 0) + pltpu.roll(w, n - half, 0)
                window = jnp.where(me == g, w, window)
                half *= 2
            span = jnp.left_shift(1, me)
            pos = lax.broadcasted_iota(jnp.int32, (small, gw), 0) + (me_sp * rows_dev - halo + i * small)
            count = jnp.minimum(pos + span, seq) - jnp.maximum(pos - span, 0)
            count = jnp.maximum(count, 1).astype(F32)
            differ = (window[pad : pad + small] / count - v[pad : pad + small]).astype(BF16)
            mixed = jnp.dot(differ, mixw[l], preferred_element_type=F32) * gain[l]
            r = pl.ds(pl.multiple_of(i * small, 16), small)
            mix_all[r, pl.ds(pl.multiple_of(me * gw, gw), gw)] = mixed.astype(BF16)

        loop(4, body6)

        pump(1)

        def msl(g):
            return mix_all.at[:, pl.ds(pl.multiple_of(g * gw, gw), gw)]

        c_x = remote(msl(me), msl(me), asend.at[2], arecv.at[2], (me_sp, xo))
        c_s = remote(msl(me), msl(me), asend.at[3], arecv.at[3], (me_sp, sib))
        c_x.start()
        c_s.start()
        pump(1)
        c_r = remote(msl(xo), msl(xo), asend.at[4], arecv.at[4], (me_sp, sib))
        remote(msl(xo), msl(xo), asend.at[2], arecv.at[2], (me_sp, xo)).wait_recv()
        c_r.start()
        need(2 * l + 1)
        remote(msl(sib), msl(sib), asend.at[3], arecv.at[3], (me_sp, sib)).wait_recv()
        dia = (1 - xid) * 2 + (1 - core)
        remote(msl(dia), msl(dia), asend.at[4], arecv.at[4], (me_sp, sib)).wait_recv()

        def body7(i):
            r = pl.ds(pl.multiple_of(i * small, 16), small)
            branch = jnp.dot(mix_all[r, :], out_all[l], preferred_element_type=F32)
            res = alpha * strm[r, :].astype(F32) + branch
            resid[r, :] = res
            sq = res * res
            a = res[:, 0:128]
            b = sq[:, 0:128]
            for k in range(1, feat // 128):
                a = a + res[:, k * 128 : (k + 1) * 128]
                b = b + sq[:, k * 128 : (k + 1) * 128]
            lanes[0, r, :] = a
            lanes[1, r, :] = b

        loop(4, body7)
        for k in range(sb):
            for q in range(2):
                blk = lanes[q, k * 128 : (k + 1) * 128, :]
                stat_send[k : k + 1, q * 128 : (q + 1) * 128] = jnp.sum(blk.T, axis=0, keepdims=True)
        stats = []
        for d in range(1, n_tp):
            c = remote(
                stat_send, stat_recv.at[d - 1], asend.at[4 + d], arecv.at[4 + d], (me_sp, (me + d) % n_tp)
            )
            c.start()
            stats.append(c)
        pump(2)
        for c in stats:
            c.wait_recv()
        total = stat_send[...]
        for d in range(1, n_tp):
            total = total + stat_recv[d - 1]
        mean = total[:, 0:128] / model
        var = total[:, 128:256] / model - mean * mean
        rstd = lax.rsqrt(var + norm_eps)
        for k in range(sb):
            mean_col[k * 128 : (k + 1) * 128, :] = jnp.broadcast_to(mean[k : k + 1, :], (128, 128)).T
            rstd_col[k * 128 : (k + 1) * 128, :] = jnp.broadcast_to(rstd[k : k + 1, :], (128, 128)).T

        def normed(r, k):
            ks = pl.ds(k * 128, 128)
            t = (resid[r, ks] - mean_col[r, :]) * rstd_col[r, :]
            return (t * ngain[l, :, ks] + nbias[l, :, ks]).astype(BF16)

        last = l == layers - 1

        def body8(i):
            if last:
                r = pl.ds(pl.multiple_of(halo + i * out_tile, 16), out_tile)
                o = pl.ds(pl.multiple_of(i * out_tile, 16), out_tile)
            else:
                r = pl.ds(pl.multiple_of(i * small, 16), small)
            for k in range(feat // 128):
                if last:
                    out[o, pl.ds(k * 128, 128)] = normed(r, k)
                else:
                    strm[r, pl.ds(k * 128, 128)] = normed(r, k)

        loop(4, body8)
        for c in [cpart, cpx, c_x, c_s, c_r] + stats:
            c.wait_send()

    @pl.when(me_sp < n_sp - 1)
    def _():
        halo_up().wait_send()

    @pl.when(me_sp > 0)
    def _():
        halo_down().wait_send()

    for b in range(blocks):
        drain(b)


def in_one_kernel(n_sp, n_tp, tokens, in_proj, group_mix, pool_gain, out_proj, norm_gain, norm_bias):
    rows_dev, feat = tokens.shape
    layers = in_proj.shape[0]
    gw = group_mix.shape[2]
    width = in_proj.shape[2] * n_sp
    ydim = 2
    halo = -(-layers * (max(pool_windows) // 2) // 32) * 32
    rows = rows_dev + 2 * halo
    rows_pad = -(-rows // 128) * 128
    me = lax.axis_index("tp")
    mixw = lax.dynamic_index_in_dim(group_mix, me, axis=1, keepdims=False)
    gain = lax.dynamic_slice_in_dim(pool_gain, me * gw, gw, axis=1)[:, None, :]
    pad = max(pool_windows) // 2
    vmem = pl.BlockSpec(memory_space=pltpu.VMEM)
    zdim = n_sp // ydim
    blocks = 2 * layers
    return pl.pallas_call(
        functools.partial(mixer_kernel, (n_sp, n_tp, ydim, halo)),
        out_shape=jax.ShapeDtypeStruct((rows_dev, feat), BF16),
        in_specs=[vmem] * 7,
        out_specs=vmem,
        scratch_shapes=[
            pltpu.VMEM((layers, feat, width), BF16),
            pltpu.VMEM((layers, width, feat), BF16),
            pltpu.VMEM((rows, feat), BF16),
            pltpu.VMEM((2, rows, gw), BF16),
            pltpu.VMEM((2, rows, gw), BF16),
            pltpu.VMEM((rows, gw), BF16),
            pltpu.VMEM((rows, gw), BF16),
            pltpu.VMEM((rows + 2 * pad, gw), F32),
            pltpu.VMEM((rows, width), BF16),
            pltpu.VMEM((rows, feat), F32),
            pltpu.VMEM((2, rows_pad, 128), F32),
            pltpu.VMEM((-(-rows_pad // 1024) * 8, 256), F32),
            pltpu.VMEM((n_tp - 1, -(-rows_pad // 1024) * 8, 256), F32),
            pltpu.VMEM((rows_pad, 128), F32),
            pltpu.VMEM((rows_pad, 128), F32),
            pltpu.SemaphoreType.DMA((blocks, 3, n_sp)),
            pltpu.SemaphoreType.DMA((blocks, n_sp)),
            pltpu.SemaphoreType.DMA((2,)),
            pltpu.SemaphoreType.DMA((2,)),
            pltpu.SemaphoreType.DMA((4 + n_tp,)),
            pltpu.SemaphoreType.DMA((4 + n_tp,)),
        ],
        compiler_params=pltpu.CompilerParams(
            collective_id=0, has_side_effects=True, vmem_limit_bytes=60 * 1024 * 1024
        ),
    )(tokens, in_proj, mixw, gain, out_proj, norm_gain[:, None, :], norm_bias[:, None, :])


def one_kernel_fits(n_sp, n_tp, tokens, in_proj, group_mix):
    rows_dev = tokens.shape[0] // n_sp
    return (
        n_tp == 4
        and group_mix.shape[1] == n_tp
        and in_proj.shape[2] == n_tp * group_mix.shape[2]
        and group_mix.shape[2] % 128 == 0
        and n_sp % 2 == 0
        and (in_proj.shape[2] // n_sp) % 128 == 0
        and rows_dev % 64 == 0
        and (tokens.shape[1] // n_tp) % 128 == 0
    )


def solution(mesh):
    in_specs = (
        P("sp", "tp"),
        P(None, "tp", "sp"),
        P(),
        P(),
        P(None, "sp", "tp"),
        P(None, "tp"),
        P(None, "tp"),
    )
    out_specs = P("sp", "tp")
    n_sp, n_tp = mesh.shape["sp"], mesh.shape["tp"]

    def run(tokens, in_proj, group_mix, *rest):
        body = on_device
        if one_kernel_fits(n_sp, n_tp, tokens, in_proj, group_mix):
            body = functools.partial(in_one_kernel, n_sp, n_tp)
        return jax.shard_map(
            body, mesh=mesh, in_specs=in_specs, out_specs=out_specs, check_vma=False
        )(tokens, in_proj, group_mix, *rest)

    return run
```
